32 devices in a mesh: fs: 8 (over z, x), tp: 4 (over y, core).
Axes of the slice: x: 2, y: 2, z: 4, core: 2. Of those that a mesh axis runs over, the one named last changes fastest.
Arguments:
- tokens: bfloat16 [64, 2048], P(('fs', 'tp')), may hold values from -6 to 6
- route_experts: int32 [64, 2], P(('fs', 'tp')), may hold values from 0 to 3, as said below
- route_logits: float32 [64, 2], P(('fs', 'tp')), may hold values from -8 to 8
- norm_gain: float32 [2048], P('fs'), may hold values from 0.1 to 1.9
- gate_train: float32 [4, 2048, 8192], P(None, 'fs', 'tp'), may hold values from -0.125 to 0.125
- up_train: float32 [4, 2048, 8192], P(None, 'fs', 'tp'), may hold values from -0.125 to 0.125
- down_train: float32 [4, 2048, 8192], P(None, 'fs', 'tp'), may hold values from -0.125 to 0.125
Outputs:
- gate_serve: bfloat16 [8, 2048, 4096], P('fs')
- up_serve: bfloat16 [8, 2048, 4096], P('fs')
- down_serve: bfloat16 [8, 2048, 4096], P('fs')
- mixed: bfloat16 [64, 2048], P(('fs', 'tp'))
The draws below stay inside these ranges and needn't reach their ends.
Inputs may be any that keep to these rules, and one draw needn't show every extreme that they name: `route_experts`: the two experts of a row differ; any expert may be named by every row of the devices that share one index along tp, and in every draw some expert is.
All inputs are finite; a program needn't handle non-finite values.
Results may differ from the reference program's by a relative error of at most 0.0085.
Values may be sent and summed in bfloat16 or wider, within the bound.
A program may use at most 192 MiB of HBM per device.

```python
import jax
import jax.numpy as jnp
from jax import lax

D = 2048
FF = 8192
EXPERTS = 4
TOK_DEV = 2
TOKENS = 64
SLICES = 2
N_TP = 4


def draw_route_experts(key, part):
    keys = jax.random.split(key, 7)
    positions = jnp.arange(TOKENS, dtype=jnp.int32)
    group_index = positions // TOK_DEV % N_TP
    favour = jax.random.randint(keys[0], (N_TP,), 0, EXPERTS, dtype=jnp.int32)
    full_group = jax.random.randint(keys[1], (), 0, N_TP, dtype=jnp.int32)
    share = jax.random.randint(keys[2], (N_TP,), 40, 91, dtype=jnp.int32)
    share = jnp.where(jnp.arange(N_TP, dtype=jnp.int32) == full_group, 100, share)
    picked = jax.random.randint(keys[3], (TOKENS,), 0, 100, dtype=jnp.int32)
    others = jax.random.randint(keys[4], (TOKENS,), 0, EXPERTS, dtype=jnp.int32)
    first = jnp.where(picked < share[group_index], favour[group_index], others)
    offset = jax.random.randint(keys[5], (TOKENS,), 1, EXPERTS, dtype=jnp.int32)
    second = (first + offset) % EXPERTS
    flipped = jax.random.randint(keys[6], (TOKENS,), 0, 2, dtype=jnp.int32)
    column_a = jnp.where(flipped == 1, second, first)
    column_b = jnp.where(flipped == 1, first, second)
    return jnp.stack([column_a, column_b], axis=1).astype(jnp.int32)


def block_scale(stream_key, shape, pieces, low, largest):
    loudness = 1.0
    for position, parts in pieces:
        heights = jax.random.uniform(jax.random.fold_in(jax.random.fold_in(stream_key, 6), position), (parts,), jnp.float32, low / len(pieces), largest / len(pieces))
        loudness = loudness * jnp.repeat(jnp.exp(heights), shape[position] // parts).reshape((-1,) + (1,) * (len(shape) - 1 - position))
    return loudness


def scatter_about(stream_key, dims, scale, most, cuts=(), kind=jnp.bfloat16):
    gain = block_scale(stream_key, dims, cuts, -0.22, 0.18) if cuts else 1.0
    array = jax.random.normal(stream_key, dims, jnp.float32) * scale * gain
    return jnp.minimum(jnp.maximum(array, -most), most).astype(kind)


def setup_inputs(seed: int = 0) -> dict:
    streams_of = jax.random.split(jax.random.key(seed), 8)
    tokens = scatter_about(streams_of[0], (TOKENS, D), 1.0, 6.0, ((0, 32),))
    route_experts = draw_route_experts(jax.random.fold_in(streams_of[7], 71), 0)
    route_logits = scatter_about(streams_of[2], (TOKENS, 2), 2.0, 8.0, ((0, 32),), jnp.float32)
    norm_gain = jnp.clip(1.0 + 0.18 * jax.random.normal(streams_of[3], (D,), jnp.float32), 0.1, 1.9)
    gate_train = scatter_about(streams_of[4], (EXPERTS, D, FF), D ** -0.5, 0.125, ((1, 8), (2, 4)), jnp.float32)
    up_train = scatter_about(streams_of[5], (EXPERTS, D, FF), D ** -0.5, 0.125, ((1, 8), (2, 4)), jnp.float32)
    down_train = scatter_about(streams_of[6], (EXPERTS, D, FF), (FF // 4) ** -0.5, 0.125, ((1, 8), (2, 4)), jnp.float32)
    return {"tokens": tokens, "route_experts": route_experts, "route_logits": route_logits, "norm_gain": norm_gain, "gate_train": gate_train, "up_train": up_train, "down_train": down_train}


def relayout(matrix):
    count, width, hidden = matrix.shape
    blocks = matrix.reshape(count, width, SLICES, hidden // SLICES)
    return blocks.transpose(0, 2, 1, 3).reshape(count * SLICES, width, hidden // SLICES)

def normalize(tokens):
    values = tokens.astype(jnp.float32)
    row_mean = lax.optimization_barrier(jnp.mean(values, axis=-1, keepdims=True))
    centered = values - row_mean
    row_var = lax.optimization_barrier(jnp.mean(centered * centered, axis=-1, keepdims=True))
    return (centered * lax.rsqrt(row_var + 1e-05)).astype(jnp.bfloat16)

def route_table(route_experts, route_logits):
    first = jax.nn.sigmoid(route_logits[:, 0] - route_logits[:, 1])
    second = jax.nn.sigmoid(route_logits[:, 1] - route_logits[:, 0])
    labels = jnp.arange(EXPERTS, dtype=jnp.int32)
    table = first[:, None] * (route_experts[:, 0:1] == labels[None, :]).astype(jnp.float32)
    table = table + second[:, None] * (route_experts[:, 1:2] == labels[None, :]).astype(jnp.float32)
    return table.astype(jnp.bfloat16)

def reference(tokens, route_experts, route_logits, norm_gain, gate_train, up_train, down_train):
    gate_new = (norm_gain[None, :, None] * gate_train).astype(jnp.bfloat16)
    up_new = (norm_gain[None, :, None] * up_train).astype(jnp.bfloat16)
    down_new = down_train.astype(jnp.bfloat16)
    normed = normalize(tokens)
    table = route_table(route_experts, route_logits)
    total = jnp.zeros((tokens.shape[0], tokens.shape[1]), jnp.float32)
    for expert in range(EXPERTS):
        gate_act = jnp.dot(normed, gate_new[expert], preferred_element_type=jnp.float32)
        up_act = jnp.dot(normed, up_new[expert], preferred_element_type=jnp.float32)
        weight = table[:, expert].astype(jnp.float32)[:, None]
        hidden = (weight * jax.nn.silu(gate_act) * up_act).astype(jnp.bfloat16)
        total = total + jnp.dot(hidden, down_new[expert].T, preferred_element_type=jnp.float32)
    return (relayout(gate_new), relayout(up_new), relayout(down_new), total.astype(jnp.bfloat16))
```

```python
import functools

import jax
import jax.numpy as jnp
from jax import lax
from jax.experimental import pallas as pl
from jax.experimental.pallas import tpu as pltpu
from jax.sharding import PartitionSpec as P

MESH = pl.DeviceIdType.MESH
PARTS = 2
LAG_TP = 2
LAG_FS = 4


def for_sending(array):
    return jax.tree.map(lambda a: a.astype(jnp.bfloat16) if a.dtype == jnp.float32 else a, array)


def normalize(tokens):
    values = tokens.astype(jnp.float32)
    row_mean = jnp.mean(values, axis=-1, keepdims=True)
    centered = values - row_mean
    row_var = jnp.mean(centered * centered, axis=-1, keepdims=True)
    return (centered * lax.rsqrt(row_var + 1e-05)).astype(jnp.bfloat16)


def per_device_general(tokens, route_experts, route_logits, norm_gain, gate_train, up_train, down_train):
    fs_size = lax.axis_size("fs")
    tp_size = lax.axis_size("tp")
    expert_count = gate_train.shape[0]
    slices = fs_size // expert_count
    scale = norm_gain[None, :, None]
    gate_half = (scale * gate_train).astype(jnp.bfloat16)
    up_half = (scale * up_train).astype(jnp.bfloat16)
    down_half = down_train.astype(jnp.bfloat16)
    swapped = (
        lax.all_to_all(gate_half, "tp", split_axis=1, concat_axis=2, tiled=True),
        lax.all_to_all(up_half, "tp", split_axis=1, concat_axis=2, tiled=True),
        lax.all_to_all(down_half, "tp", split_axis=1, concat_axis=2, tiled=True),
    )
    quarter = swapped[0].shape[1]
    hidden_total = swapped[0].shape[2]
    block_width = hidden_total // slices

    def split_quarter(matrix):
        blocks = matrix.reshape(expert_count, quarter, slices, block_width)
        return blocks.transpose(0, 2, 1, 3).reshape(expert_count * slices, quarter, block_width)

    owned = lax.all_to_all(
        for_sending(tuple((split_quarter(matrix) for matrix in swapped))),
        "fs",
        split_axis=0,
        concat_axis=1,
        tiled=True,
    )
    stacked = tuple((matrix.reshape(1, fs_size, 1, quarter, block_width) for matrix in owned))
    joined = jax.tree.map(
        lambda part, own: part.astype(own.dtype),
        lax.all_gather(for_sending(stacked), "tp", axis=2, tiled=True),
        stacked,
    )
    gate_serve, up_serve, down_serve = tuple(
        (matrix.reshape(1, fs_size * tp_size * quarter, block_width) for matrix in joined)
    )
    normed = normalize(tokens)
    first = jax.nn.sigmoid(route_logits[:, 0] - route_logits[:, 1])
    second = jax.nn.sigmoid(route_logits[:, 1] - route_logits[:, 0])
    labels = jnp.arange(expert_count, dtype=jnp.int32)
    table = first[:, None] * (route_experts[:, 0:1] == labels[None, :]).astype(jnp.float32)
    table = table + second[:, None] * (route_experts[:, 1:2] == labels[None, :]).astype(jnp.float32)
    table = table.astype(jnp.bfloat16)
    rows_all, table_all = (
        lax.all_gather(normed, "fs", axis=0, tiled=True),
        lax.all_gather(table, "fs", axis=0, tiled=True),
    )
    own_expert = lax.axis_index("fs") // slices
    selector = (labels == own_expert).astype(jnp.float32)
    weight = jnp.sum(table_all.astype(jnp.float32) * selector[None, :], axis=1)
    gate_act = jnp.dot(rows_all, gate_serve[0], preferred_element_type=jnp.float32)
    up_act = jnp.dot(rows_all, up_serve[0], preferred_element_type=jnp.float32)
    hidden = (weight[:, None] * jax.nn.silu(gate_act) * up_act).astype(jnp.bfloat16)
    down_own = down_serve[0]
    summed = lax.psum_scatter(
        lax.dot_general(
            hidden, down_own, (((1,), (1,)), ((), ())), preferred_element_type=jnp.float32
        ),
        "fs",
        scatter_dimension=0,
        tiled=True,
    )
    return (gate_serve, up_serve, down_serve, summed.astype(jnp.bfloat16))


def round_kernel(gain_ref, gate_ref, up_ref, down_ref, out_ref):
    gain = gain_ref[...]
    out_ref[0, 0] = (gain * gate_ref[0]).astype(jnp.bfloat16)
    out_ref[1, 0] = (gain * up_ref[0]).astype(jnp.bfloat16)
    out_ref[2, 0] = down_ref[0].astype(jnp.bfloat16)


def rounded(norm_gain, gate_train, up_train, down_train):
    experts, rows, width = gate_train.shape
    tile = rows // 2
    weight = pl.BlockSpec((1, tile, width), lambda e, r: (e, r, 0))
    return pl.pallas_call(
        round_kernel,
        grid=(experts, rows // tile),
        in_specs=[pl.BlockSpec((tile, 1), lambda e, r: (r, 0)), weight, weight, weight],
        out_specs=pl.BlockSpec((3, 1, tile, width), lambda e, r: (0, e, r, 0)),
        out_shape=jax.ShapeDtypeStruct((3, experts, rows, width), jnp.bfloat16),
        name="round_weights",
    )(norm_gain[:, None], gate_train, up_train, down_train)


def exchange_kernel(
    src, joined, transit, held, l_in, l_out, z_s, z_r, y_s, y_r, x_s, x_r, c_s, c_r
):
    matrices, experts, rows, width = src.shape
    chunk = rows // PARTS
    pieces = matrices * PARTS * experts
    f = lax.axis_index("fs")
    t = lax.axis_index("tp")
    z, x = lax.div(f, 2), lax.rem(f, 2)
    s, c = lax.div(t, 2), lax.rem(t, 2)
    y_peer = (f, (1 - s) * 2 + c)
    c_peer = (f, s * 2 + 1 - c)
    x_peer = (z * 2 + 1 - x, t)

    def z_peer(d):
        return (lax.rem(z + d, experts) * 2 + x, t)

    barrier = pltpu.get_barrier_semaphore()
    for d in range(1, experts):
        pl.semaphore_signal(barrier, inc=1, device_id=z_peer(d), device_id_type=MESH)
    for peer in (y_peer, c_peer, x_peer):
        pl.semaphore_signal(barrier, inc=1, device_id=peer, device_id_type=MESH)

    def parts_of(k):
        d = lax.rem(k, experts)
        g = lax.div(k, experts)
        return d, g, lax.rem(g, PARTS), lax.div(g, PARTS)

    def final(m, zs, xs, h):
        row = pl.multiple_of((zs * 2 + xs) * rows + h * chunk, chunk)
        return joined.at[m, pl.ds(row, chunk), pl.ds(pl.multiple_of(c * width, width), width)]

    def passing(m, zs, h):
        return transit.at[m, zs, pl.ds(pl.multiple_of(h * chunk, chunk), chunk)]

    def source(m, e, h):
        return src.at[m, e, pl.ds(pl.multiple_of(h * chunk, chunk), chunk)]

    def remote(a, b, send, recv, peer):
        return pltpu.make_async_remote_copy(
            src_ref=a, dst_ref=b, send_sem=send, recv_sem=recv, device_id=peer,
            device_id_type=MESH,
        )

    def load(g):
        return pltpu.make_async_copy(
            source(lax.div(g, PARTS), z, lax.rem(g, PARTS)), held.at[g], l_in.at[g]
        )

    @pl.loop(0, matrices * PARTS)
    def _(g):
        load(g).start()

    pl.semaphore_wait(barrier, experts + 2)

    def send_z(home):
        @pl.loop(0, pieces)
        def _(k):
            d, g, h, m = parts_of(k)

            @pl.when(d > 0)
            def _():
                here = final(m, z, x, h) if home else passing(m, z, h)
                there = source(m, lax.rem(z + d, experts), h)
                remote(there, here, z_s.at[k], z_r.at[k], z_peer(d)).start()

            @pl.when(d == 0)
            def _():
                here = final(m, z, x, h) if home else passing(m, z, h)
                load(g).wait()
                pltpu.make_async_copy(held.at[g], here, l_out.at[g]).start()

    def place(k, keep):
        d, g, h, m = parts_of(k)
        zs = lax.rem(z + experts - d, experts)
        return final(m, zs, x, h) if keep else passing(m, zs, h)

    def forward(k, keep):
        d, g, h, m = parts_of(k)
        zs = lax.rem(z + experts - d, experts)
        if keep:
            here = final(m, zs, x, h)
            remote(here, here, c_s.at[k], c_r.at[k], c_peer).start()
        else:
            remote(
                passing(m, zs, h), final(m, zs, x, h), x_s.at[k], x_r.at[k], x_peer
            ).start()

    def run(home):
        send_z(home)

        @pl.loop(0, pieces + LAG_FS)
        def _(i):
            @pl.when(i < pieces)
            def _():
                d, g, h, m = parts_of(i)
                here = place(i, home)

                @pl.when(d > 0)
                def _():
                    remote(here, here, z_s.at[i], z_r.at[i], y_peer).wait_recv()

                @pl.when(d == 0)
                def _():
                    pltpu.make_async_copy(held.at[g], here, l_out.at[g]).wait()

                remote(here, here, y_s.at[i], y_r.at[i], y_peer).start()
                forward(i, home)

            @pl.when((i >= LAG_TP) & (i < pieces + LAG_TP))
            def _():
                k = i - LAG_TP
                here = place(k, not home)
                remote(here, here, y_s.at[k], y_r.at[k], y_peer).wait_recv()
                forward(k, not home)

            @pl.when(i >= LAG_FS)
            def _():
                k = i - LAG_FS
                d, g, h, m = parts_of(k)
                here = final(m, lax.rem(z + experts - d, experts), 1 - x, h)
                remote(here, here, x_s.at[k], x_r.at[k], x_peer).wait_recv()
                remote(
                    here, here, c_s.at[pieces + k], c_r.at[pieces + k], c_peer
                ).start()

        @pl.loop(0, pieces)
        def _(k):
            d, g, h, m = parts_of(k)
            zs = lax.rem(z + experts - d, experts)
            here = place(k, home)

            @pl.when(d > 0)
            def _():
                remote(
                    source(m, lax.rem(z + d, experts), h), here, z_s.at[k], z_r.at[k], y_peer
                ).wait_send()

            remote(here, here, y_s.at[k], y_r.at[k], y_peer).wait_send()
            remote(passing(m, zs, h), here, x_s.at[k], x_r.at[k], x_peer).wait_send()
            for q in range(2):
                xs = x if q == 0 else 1 - x
                mine = final(m, zs, xs, h)
                row = pl.multiple_of((zs * 2 + xs) * rows + h * chunk, chunk)
                other = joined.at[
                    m, pl.ds(row, chunk), pl.ds(pl.multiple_of((1 - c) * width, width), width)
                ]
                n = q * pieces + k
                remote(mine, other, c_s.at[n], c_r.at[n], c_peer).wait()

    @pl.when(s == x)
    def _():
        run(True)

    @pl.when(s != x)
    def _():
        run(False)


def exchanged(packed, fs_size):
    matrices, experts, rows, width = packed.shape
    pieces = matrices * PARTS * experts
    groups = matrices * PARTS
    anywhere = pl.BlockSpec(memory_space=pl.ANY)
    dma = pltpu.SemaphoreType.DMA
    return pl.pallas_call(
        exchange_kernel,
        in_specs=[anywhere],
        out_specs=[anywhere, anywhere],
        out_shape=[
            jax.ShapeDtypeStruct((matrices, fs_size * rows, 2 * width), jnp.bfloat16),
            jax.ShapeDtypeStruct(packed.shape, jnp.bfloat16),
        ],
        scratch_shapes=[
            pltpu.VMEM((groups, rows // PARTS, width), jnp.bfloat16),
            dma((groups,)),
            dma((groups,)),
            dma((pieces,)),
            dma((pieces,)),
            dma((pieces,)),
            dma((pieces,)),
            dma((pieces,)),
            dma((pieces,)),
            dma((2 * pieces,)),
            dma((2 * pieces,)),
        ],
        compiler_params=pltpu.CompilerParams(collective_id=0, has_side_effects=True),
        name="exchange_weights",
    )(packed)[0]


def expert_kernel(rows_ref, weight_ref, joined_ref, gate_ref, up_ref, down_ref, sum_ref):
    @pl.when(pl.program_id(0) == 0)
    def _():
        sum_ref[...] = jnp.zeros_like(sum_ref)

    gate_ref[0] = joined_ref[0]
    up_ref[0] = joined_ref[1]
    down_ref[0] = joined_ref[2]
    rows = rows_ref[...]
    gate_act = jnp.dot(rows, joined_ref[0], preferred_element_type=jnp.float32)
    up_act = jnp.dot(rows, joined_ref[1], preferred_element_type=jnp.float32)
    hidden = (weight_ref[...] * jax.nn.silu(gate_act) * up_act).astype(jnp.bfloat16)
    sum_ref[...] += lax.dot_general(
        hidden, joined_ref[2], (((1,), (1,)), ((), ())), preferred_element_type=jnp.float32
    )


def expert_block(rows_all, weight, joined):
    matrices, depth, width = joined.shape
    tile = width // 8
    count = rows_all.shape[0]
    serve = jax.ShapeDtypeStruct((1, depth, width), jnp.bfloat16)
    block = pl.BlockSpec((1, depth, tile), lambda i: (0, 0, i))
    whole = lambda i: (0, 0)
    return pl.pallas_call(
        expert_kernel,
        grid=(width // tile,),
        in_specs=[
            pl.BlockSpec((count, depth), whole),
            pl.BlockSpec((count, 1), whole),
            pl.BlockSpec((matrices, depth, tile), lambda i: (0, 0, i)),
        ],
        out_specs=[block, block, block, pl.BlockSpec((count, depth), whole)],
        out_shape=[serve, serve, serve, jax.ShapeDtypeStruct((count, depth), jnp.float32)],
        name="expert_block",
    )(rows_all, weight, joined)


def per_device(tokens, route_experts, route_logits, norm_gain, gate_train, up_train, down_train):
    fs_size = lax.axis_size("fs")
    expert_count = gate_train.shape[0]
    slices = fs_size // expert_count
    normed = normalize(tokens)
    first = jax.nn.sigmoid(route_logits[:, 0] - route_logits[:, 1])
    second = jax.nn.sigmoid(route_logits[:, 1] - route_logits[:, 0])
    labels = jnp.arange(expert_count, dtype=jnp.int32)
    table = first[:, None] * (route_experts[:, 0:1] == labels[None, :]).astype(jnp.float32)
    table = table + second[:, None] * (route_experts[:, 1:2] == labels[None, :]).astype(jnp.float32)
    table = table.astype(jnp.bfloat16)
    rows_all, table_all = (
        lax.all_gather(normed, "fs", axis=0, tiled=True),
        lax.all_gather(table, "fs", axis=0, tiled=True),
    )
    own_expert = lax.axis_index("fs") // slices
    selector = (labels == own_expert).astype(jnp.float32)
    weight = jnp.sum(table_all.astype(jnp.float32) * selector[None, :], axis=1)
    joined = exchanged(rounded(norm_gain, gate_train, up_train, down_train), fs_size)
    gate_serve, up_serve, down_serve, partial = expert_block(rows_all, weight[:, None], joined)
    summed = lax.psum_scatter(partial, "fs", scatter_dimension=0, tiled=True)
    return (gate_serve, up_serve, down_serve, summed.astype(jnp.bfloat16))


def two_by_two(fs_size, tp_size, experts):
    return fs_size == 2 * experts and tp_size == 4


def choose(*args):
    fits = two_by_two(lax.axis_size("fs"), lax.axis_size("tp"), args[4].shape[0])
    return (per_device if fits else per_device_general)(*args)


def solution(mesh):
    return jax.shard_map(
        choose,
        mesh=mesh,
        in_specs=(
            P(("fs", "tp"), None),
            P(("fs", "tp"), None),
            P(("fs", "tp"), None),
            P("fs"),
            P(None, "fs", "tp"),
            P(None, "fs", "tp"),
            P(None, "fs", "tp"),
        ),
        out_specs=(
            P("fs", None, None),
            P("fs", None, None),
            P("fs", None, None),
            P(("fs", "tp"), None),
        ),
        check_vma=False,
    )
```

```python
import functools

import jax
import jax.numpy as jnp
from jax import lax
from jax.experimental import pallas as pl
from jax.experimental.pallas import tpu as pltpu
from jax.sharding import PartitionSpec as P

MESH = pl.DeviceIdType.MESH
PARTS = 4
LAG_TP = 3
LAG_FS = 6
PAD = 128


def for_sending(array):
    return jax.tree.map(lambda a: a.astype(jnp.bfloat16) if a.dtype == jnp.float32 else a, array)


def normalize(tokens):
    values = tokens.astype(jnp.float32)
    row_mean = jnp.mean(values, axis=-1, keepdims=True)
    centered = values - row_mean
    row_var = jnp.mean(centered * centered, axis=-1, keepdims=True)
    return (centered * lax.rsqrt(row_var + 1e-05)).astype(jnp.bfloat16)


def per_device_general(tokens, route_experts, route_logits, norm_gain, gate_train, up_train, down_train):
    fs_size = lax.axis_size("fs")
    tp_size = lax.axis_size("tp")
    expert_count = gate_train.shape[0]
    slices = fs_size // expert_count
    scale = norm_gain[None, :, None]
    gate_half = (scale * gate_train).astype(jnp.bfloat16)
    up_half = (scale * up_train).astype(jnp.bfloat16)
    down_half = down_train.astype(jnp.bfloat16)
    swapped = (
        lax.all_to_all(gate_half, "tp", split_axis=1, concat_axis=2, tiled=True),
        lax.all_to_all(up_half, "tp", split_axis=1, concat_axis=2, tiled=True),
        lax.all_to_all(down_half, "tp", split_axis=1, concat_axis=2, tiled=True),
    )
    quarter = swapped[0].shape[1]
    hidden_total = swapped[0].shape[2]
    block_width = hidden_total // slices

    def split_quarter(matrix):
        blocks = matrix.reshape(expert_count, quarter, slices, block_width)
        return blocks.transpose(0, 2, 1, 3).reshape(expert_count * slices, quarter, block_width)

    owned = lax.all_to_all(
        for_sending(tuple((split_quarter(matrix) for matrix in swapped))),
        "fs",
        split_axis=0,
        concat_axis=1,
        tiled=True,
    )
    stacked = tuple((matrix.reshape(1, fs_size, 1, quarter, block_width) for matrix in owned))
    joined = jax.tree.map(
        lambda part, own: part.astype(own.dtype),
        lax.all_gather(for_sending(stacked), "tp", axis=2, tiled=True),
        stacked,
    )
    gate_serve, up_serve, down_serve = tuple(
        (matrix.reshape(1, fs_size * tp_size * quarter, block_width) for matrix in joined)
    )
    normed = normalize(tokens)
    first = jax.nn.sigmoid(route_logits[:, 0] - route_logits[:, 1])
    second = jax.nn.sigmoid(route_logits[:, 1] - route_logits[:, 0])
    labels = jnp.arange(expert_count, dtype=jnp.int32)
    table = first[:, None] * (route_experts[:, 0:1] == labels[None, :]).astype(jnp.float32)
    table = table + second[:, None] * (route_experts[:, 1:2] == labels[None, :]).astype(jnp.float32)
    table = table.astype(jnp.bfloat16)
    rows_all, table_all = (
        lax.all_gather(normed, "fs", axis=0, tiled=True),
        lax.all_gather(table, "fs", axis=0, tiled=True),
    )
    own_expert = lax.axis_index("fs") // slices
    selector = (labels == own_expert).astype(jnp.float32)
    weight = jnp.sum(table_all.astype(jnp.float32) * selector[None, :], axis=1)
    gate_act = jnp.dot(rows_all, gate_serve[0], preferred_element_type=jnp.float32)
    up_act = jnp.dot(rows_all, up_serve[0], preferred_element_type=jnp.float32)
    hidden = (weight[:, None] * jax.nn.silu(gate_act) * up_act).astype(jnp.bfloat16)
    down_own = down_serve[0]
    summed = lax.psum_scatter(
        lax.dot_general(
            hidden, down_own, (((1,), (1,)), ((), ())), preferred_element_type=jnp.float32
        ),
        "fs",
        scatter_dimension=0,
        tiled=True,
    )
    return (gate_serve, up_serve, down_serve, summed.astype(jnp.bfloat16))


def round_kernel(gain_ref, gate_ref, up_ref, down_ref, out_ref):
    gain = gain_ref[...]
    out_ref[0, 0] = (gain * gate_ref[0]).astype(jnp.bfloat16)
    out_ref[1, 0] = (gain * up_ref[0]).astype(jnp.bfloat16)
    out_ref[2, 0] = down_ref[0].astype(jnp.bfloat16)


def rounded(norm_gain, gate_train, up_train, down_train):
    experts, rows, width = gate_train.shape
    tile = rows // 2
    weight = pl.BlockSpec((1, tile, width), lambda e, r: (e, r, 0))
    return pl.pallas_call(
        round_kernel,
        grid=(experts, rows // tile),
        in_specs=[pl.BlockSpec((tile, 1), lambda e, r: (r, 0)), weight, weight, weight],
        out_specs=pl.BlockSpec((3, 1, tile, width), lambda e, r: (0, e, r, 0)),
        out_shape=jax.ShapeDtypeStruct((3, experts, rows, width), jnp.bfloat16),
        name="round_weights",
    )(norm_gain[:, None], gate_train, up_train, down_train)


def exchange_kernel(
    src, mine_ref, joined, transit, all_ref, held, l_in, l_out, z_s, z_r, y_s, y_r, x_s, x_r,
    c_s, c_r, g_s, g_r
):
    matrices, experts, rows, width = src.shape
    chunk = rows // PARTS
    pieces = matrices * PARTS * experts
    f = lax.axis_index("fs")
    t = lax.axis_index("tp")
    z, x = lax.div(f, 2), lax.rem(f, 2)
    s, c = lax.div(t, 2), lax.rem(t, 2)
    y_peer = (f, (1 - s) * 2 + c)
    c_peer = (f, s * 2 + 1 - c)
    x_peer = (z * 2 + 1 - x, t)

    def z_peer(d):
        return (lax.rem(z + d, experts) * 2 + x, t)

    barrier = pltpu.get_barrier_semaphore()
    fs_size = all_ref.shape[0]
    fs_peers = [(lax.rem(f + q, fs_size), t) for q in range(1, fs_size)]
    for peer in (*fs_peers, y_peer, c_peer):
        pl.semaphore_signal(barrier, inc=1, device_id=peer, device_id_type=MESH)

    def parts_of(k):
        d = lax.rem(k, experts)
        g = lax.div(k, experts)
        return d, g, lax.rem(g, PARTS), lax.div(g, PARTS)

    def final(m, zs, xs, h):
        row = pl.multiple_of((zs * 2 + xs) * rows + h * chunk, chunk)
        return joined.at[m, pl.ds(row, chunk), pl.ds(pl.multiple_of(c * width, width), width)]

    def passing(m, zs, h):
        return transit.at[m, zs, pl.ds(pl.multiple_of(h * chunk, chunk), chunk)]

    def source(m, e, h):
        return src.at[m, e, pl.ds(pl.multiple_of(h * chunk, chunk), chunk)]

    def remote(a, b, send, recv, peer):
        return pltpu.make_async_remote_copy(
            src_ref=a, dst_ref=b, send_sem=send, recv_sem=recv, device_id=peer,
            device_id_type=MESH,
        )

    def load(g):
        return pltpu.make_async_copy(
            source(lax.div(g, PARTS), z, lax.rem(g, PARTS)), held.at[g], l_in.at[g]
        )

    @pl.loop(0, matrices * PARTS)
    def _(g):
        load(g).start()

    all_ref[f] = mine_ref[...]
    pl.semaphore_wait(barrier, fs_size + 1)
    for q, peer in enumerate(fs_peers):
        remote(mine_ref, all_ref.at[f], g_s.at[q], g_r.at[q], peer).start()

    def send_z(home):
        @pl.loop(0, pieces)
        def _(k):
            d, g, h, m = parts_of(k)

            @pl.when(d > 0)
            def _():
                here = final(m, z, x, h) if home else passing(m, z, h)
                there = source(m, lax.rem(z + d, experts), h)
                remote(there, here, z_s.at[k], z_r.at[k], z_peer(d)).start()

            @pl.when(d == 0)
            def _():
                here = final(m, z, x, h) if home else passing(m, z, h)
                load(g).wait()
                pltpu.make_async_copy(held.at[g], here, l_out.at[g]).start()

    def place(k, keep):
        d, g, h, m = parts_of(k)
        zs = lax.rem(z + experts - d, experts)
        return final(m, zs, x, h) if keep else passing(m, zs, h)

    def forward(k, keep):
        d, g, h, m = parts_of(k)
        zs = lax.rem(z + experts - d, experts)
        if keep:
            here = final(m, zs, x, h)
            remote(here, here, c_s.at[k], c_r.at[k], c_peer).start()
        else:
            remote(
                passing(m, zs, h), final(m, zs, x, h), x_s.at[k], x_r.at[k], x_peer
            ).start()

    def run(home):
        send_z(home)

        @pl.loop(0, pieces + LAG_FS)
        def _(i):
            @pl.when(i < pieces)
            def _():
                d, g, h, m = parts_of(i)
                here = place(i, home)

                @pl.when(d > 0)
                def _():
                    remote(here, here, z_s.at[i], z_r.at[i], y_peer).wait_recv()

                @pl.when(d == 0)
                def _():
                    pltpu.make_async_copy(held.at[g], here, l_out.at[g]).wait()

                remote(here, here, y_s.at[i], y_r.at[i], y_peer).start()
                forward(i, home)

            @pl.when((i >= LAG_TP) & (i < pieces + LAG_TP))
            def _():
                k = i - LAG_TP
                here = place(k, not home)
                remote(here, here, y_s.at[k], y_r.at[k], y_peer).wait_recv()
                forward(k, not home)

            @pl.when(i >= LAG_FS)
            def _():
                k = i - LAG_FS
                d, g, h, m = parts_of(k)
                here = final(m, lax.rem(z + experts - d, experts), 1 - x, h)
                remote(here, here, x_s.at[k], x_r.at[k], x_peer).wait_recv()
                remote(
                    here, here, c_s.at[pieces + k], c_r.at[pieces + k], c_peer
                ).start()

        @pl.loop(0, pieces)
        def _(k):
            d, g, h, m = parts_of(k)
            zs = lax.rem(z + experts - d, experts)
            here = place(k, home)

            @pl.when(d > 0)
            def _():
                remote(
                    source(m, lax.rem(z + d, experts), h), here, z_s.at[k], z_r.at[k], y_peer
                ).wait_send()

            remote(here, here, y_s.at[k], y_r.at[k], y_peer).wait_send()
            remote(passing(m, zs, h), here, x_s.at[k], x_r.at[k], x_peer).wait_send()
            for q in range(2):
                xs = x if q == 0 else 1 - x
                mine = final(m, zs, xs, h)
                row = pl.multiple_of((zs * 2 + xs) * rows + h * chunk, chunk)
                other = joined.at[
                    m, pl.ds(row, chunk), pl.ds(pl.multiple_of((1 - c) * width, width), width)
                ]
                n = q * pieces + k
                remote(mine, other, c_s.at[n], c_r.at[n], c_peer).wait()

    @pl.when(s == x)
    def _():
        run(True)

    @pl.when(s != x)
    def _():
        run(False)

    for q, peer in enumerate(fs_peers):
        owner = lax.rem(f + fs_size - q - 1, fs_size)
        remote(mine_ref, all_ref.at[owner], g_s.at[q], g_r.at[q], peer).wait()


def exchanged(packed, mine, fs_size):
    matrices, experts, rows, width = packed.shape
    pieces = matrices * PARTS * experts
    groups = matrices * PARTS
    anywhere = pl.BlockSpec(memory_space=pl.ANY)
    in_vmem = pl.BlockSpec(memory_space=pltpu.VMEM)
    dma = pltpu.SemaphoreType.DMA
    return pl.pallas_call(
        exchange_kernel,
        in_specs=[anywhere, in_vmem],
        out_specs=[anywhere, anywhere, in_vmem],
        out_shape=[
            jax.ShapeDtypeStruct((matrices, fs_size * rows, 2 * width), jnp.bfloat16),
            jax.ShapeDtypeStruct(packed.shape, jnp.bfloat16),
            jax.ShapeDtypeStruct((fs_size, *mine.shape), jnp.bfloat16),
        ],
        scratch_shapes=[
            pltpu.VMEM((groups, rows // PARTS, width), jnp.bfloat16),
            dma((groups,)),
            dma((groups,)),
            dma((pieces,)),
            dma((pieces,)),
            dma((pieces,)),
            dma((pieces,)),
            dma((pieces,)),
            dma((pieces,)),
            dma((2 * pieces,)),
            dma((2 * pieces,)),
            dma((fs_size - 1,)),
            dma((fs_size - 1,)),
        ],
        compiler_params=pltpu.CompilerParams(collective_id=0, has_side_effects=True),
        name="exchange_weights",
    )(packed, mine)


def expert_kernel(rows_ref, weight_ref, joined_ref, gate_ref, up_ref, down_ref, sum_ref):
    @pl.when(pl.program_id(0) == 0)
    def _():
        sum_ref[...] = jnp.zeros_like(sum_ref)

    gate_ref[0] = joined_ref[0]
    up_ref[0] = joined_ref[1]
    down_ref[0] = joined_ref[2]
    rows = rows_ref[...]
    gate_act = jnp.dot(rows, joined_ref[0], preferred_element_type=jnp.float32)
    up_act = jnp.dot(rows, joined_ref[1], preferred_element_type=jnp.float32)
    hidden = (weight_ref[...] * jax.nn.silu(gate_act) * up_act).astype(jnp.bfloat16)
    sum_ref[...] += lax.dot_general(
        hidden, joined_ref[2], (((1,), (1,)), ((), ())), preferred_element_type=jnp.float32
    )


def expert_block(rows_all, weight, joined):
    matrices, depth, width = joined.shape
    tile = width // 8
    count = rows_all.shape[0]
    serve = jax.ShapeDtypeStruct((1, depth, width), jnp.bfloat16)
    block = pl.BlockSpec((1, depth, tile), lambda i: (0, 0, i))
    whole = lambda i: (0, 0)
    return pl.pallas_call(
        expert_kernel,
        grid=(width // tile,),
        in_specs=[
            pl.BlockSpec((count, depth), whole),
            pl.BlockSpec((count, 1), whole),
            pl.BlockSpec((matrices, depth, tile), lambda i: (0, 0, i)),
        ],
        out_specs=[block, block, block, pl.BlockSpec((count, depth), whole)],
        out_shape=[serve, serve, serve, jax.ShapeDtypeStruct((count, depth), jnp.float32)],
        name="expert_block",
    )(rows_all, weight, joined)


def reduce_kernel(part_ref, out_ref, landed, send, recv):
    f = lax.axis_index("fs")
    t = lax.axis_index("tp")
    fs_size = part_ref.shape[0]
    peers = [lax.rem(f + q, fs_size) for q in range(1, fs_size)]
    barrier = pltpu.get_barrier_semaphore()
    for peer in peers:
        pl.semaphore_signal(barrier, inc=1, device_id=(peer, t), device_id_type=MESH)
    pl.semaphore_wait(barrier, fs_size - 1)

    def copy(q, slot):
        return pltpu.make_async_remote_copy(
            src_ref=part_ref.at[peers[q]], dst_ref=landed.at[slot], send_sem=send.at[q],
            recv_sem=recv.at[q], device_id=(peers[q], t), device_id_type=MESH,
        )

    for q in range(fs_size - 1):
        copy(q, q).start()
    total = part_ref[f]
    for q in range(fs_size - 1):
        copy(q, q).wait()
        total = total + landed[q]
    out_ref[...] = total.astype(out_ref.dtype)


def reduced(part):
    fs_size, count, depth = part.shape
    in_vmem = pl.BlockSpec(memory_space=pltpu.VMEM)
    return pl.pallas_call(
        reduce_kernel,
        in_specs=[in_vmem],
        out_specs=in_vmem,
        out_shape=jax.ShapeDtypeStruct((count, depth), jnp.bfloat16),
        scratch_shapes=[
            pltpu.VMEM((fs_size - 1, count, depth), jnp.float32),
            pltpu.SemaphoreType.DMA((fs_size - 1,)),
            pltpu.SemaphoreType.DMA((fs_size - 1,)),
        ],
        compiler_params=pltpu.CompilerParams(collective_id=1, has_side_effects=True),
        name="reduce_rows",
    )(part)


def per_device(tokens, route_experts, route_logits, norm_gain, gate_train, up_train, down_train):
    fs_size = lax.axis_size("fs")
    expert_count = gate_train.shape[0]
    slices = fs_size // expert_count
    normed = normalize(tokens)
    first = jax.nn.sigmoid(route_logits[:, 0] - route_logits[:, 1])
    second = jax.nn.sigmoid(route_logits[:, 1] - route_logits[:, 0])
    labels = jnp.arange(PAD, dtype=jnp.int32)
    table = first[:, None] * (route_experts[:, 0:1] == labels[None, :]).astype(jnp.float32)
    table = table + second[:, None] * (route_experts[:, 1:2] == labels[None, :]).astype(jnp.float32)
    table = table.astype(jnp.bfloat16)
    packed = rounded(norm_gain, gate_train, up_train, down_train)
    mine = jnp.concatenate([normed, table], axis=1)
    joined, _, gathered = exchanged(packed, mine, fs_size)
    count, depth = tokens.shape
    gathered = gathered.reshape(fs_size * count, depth + PAD)
    rows_all, table_all = gathered[:, :depth], gathered[:, depth:]
    own_expert = lax.axis_index("fs") // slices
    selector = (labels == own_expert).astype(jnp.float32)
    weight = jnp.sum(table_all.astype(jnp.float32) * selector[None, :], axis=1)
    gate_serve, up_serve, down_serve, partial = expert_block(rows_all, weight[:, None], joined)
    mixed = reduced(partial.reshape(fs_size, count, depth))
    return (gate_serve, up_serve, down_serve, mixed)


def two_by_two(fs_size, tp_size, experts):
    return fs_size == 2 * experts and tp_size == 4 and experts <= PAD


def choose(*args):
    fits = two_by_two(lax.axis_size("fs"), lax.axis_size("tp"), args[4].shape[0])
    return (per_device if fits else per_device_general)(*args)


def solution(mesh):
    return jax.shard_map(
        choose,
        mesh=mesh,
        in_specs=(
            P(("fs", "tp"), None),
            P(("fs", "tp"), None),
            P(("fs", "tp"), None),
            P("fs"),
            P(None, "fs", "tp"),
            P(None, "fs", "tp"),
            P(None, "fs", "tp"),
        ),
        out_specs=(
            P("fs", None, None),
            P("fs", None, None),
            P("fs", None, None),
            P(("fs", "tp"), None),
        ),
        check_vma=False,
    )
```
